32 devices in a mesh: sp: 8 (over z, y), tp: 4 (over x, core).
Axes of the slice: x: 2, y: 2, z: 4, core: 2. Of those that a mesh axis runs over, the one named last changes fastest.
Arguments:
- cotangent: bfloat16 [1024, 2048], P('sp', 'tp'), may hold values from -6 to 6
- mixer_out: bfloat16 [1024, 2048], P('sp', 'tp'), may hold values from -6 to 6
- route_ids: int32 [1024, 2], P('sp'), may hold values from 0 to 7, all different within a row; in each aligned block of 128 rows (0 to 127, 128 to 255, ...) at most 64 rows name the same one
- route_weights: float32 [1024, 2], P('sp'), may hold values from 0.2 to 1
- conv_out: bfloat16 [1024, 2048], P('sp', 'tp'), may hold values from -6 to 6
- recur_gate: bfloat16 [1024, 2048], P('sp', 'tp'), may hold values from 0.007 to 1
- input_gate: bfloat16 [1024, 2048], P('sp', 'tp'), may hold values from 0.099609375 to 0.8984375
- gate_pre: bfloat16 [1024, 2048], P('sp', 'tp'), may hold values from -6 to 6
- states_before: bfloat16 [1024, 2048], P('sp', 'tp'), may hold values from -4 to 4
- decay_rate: float32 [2048], P('tp'), may hold values from 4e-07 to 0.008
- out_proj: bfloat16 [2048, 2048], P(None, 'tp'), may hold values from -0.125 to 0.125
- recur_map: bfloat16 [4, 512, 512], P('tp'), may hold values from -0.25 to 0.25
- input_map: bfloat16 [4, 512, 512], P('tp'), may hold values from -0.25 to 0.25
- expert_gate: bfloat16 [8, 2048, 1024], P('sp', None, 'tp'), may hold values from -0.125 to 0.125
- expert_up: bfloat16 [8, 2048, 1024], P('sp', None, 'tp'), may hold values from -0.125 to 0.125
- expert_down: bfloat16 [8, 1024, 2048], P('sp', 'tp'), may hold values from -0.1875 to 0.1875
Outputs:
- grad_expert_gate: bfloat16 [8, 2048, 1024], P('sp', None, 'tp')
- grad_expert_up: bfloat16 [8, 2048, 1024], P('sp', None, 'tp')
- grad_expert_down: bfloat16 [8, 1024, 2048], P('sp', 'tp')
- grad_out_proj: float32 [2048, 2048], P('sp', 'tp')
- grad_conv: bfloat16 [1024, 2048], P('sp', 'tp')
- grad_gate_pre: bfloat16 [1024, 2048], P('sp', 'tp')
The draws below stay inside these ranges and needn't reach their ends.
Inputs may be any that keep to these rules, and one draw needn't show every extreme that they name: `route_ids`: the two experts of a token differ. In every aligned block of 128 tokens no expert is named by more than 64 routes, and in some block some expert by exactly 64.
All inputs are finite; a program needn't handle non-finite values.
Results may differ from the reference program's by a relative error of at most 0.0093.
Values may be sent and summed in bfloat16 or wider, within the bound.
A program may use at most 64 MiB of HBM per device.

```python
import math
import jax
import jax.numpy as jnp
import numpy as np
from jax import lax

D = 2048
LRU = 2048
BLOCKS = 4
BLOCK_W = 512
FF = 1024
TOK_DEV = 128
TOKENS = 1024
EXPERTS = 8
CAP = 64
N_SP = 8


def draw_recur_gate(key, part):
    key_one, key_two = jax.random.split(key)
    span_count = TOKENS // 128
    base_gate = jax.random.uniform(key_one, (TOKENS, LRU), jnp.float32, 0.5, 1.0)
    factor = jnp.exp(jax.random.uniform(key_two, (span_count, 1, 1), jnp.float32, math.log(0.15), 0.0))
    return (base_gate.reshape(span_count, 128, LRU) * factor).reshape(TOKENS, LRU).astype(jnp.bfloat16)


def draw_decay_rate(key, part):
    key_one, key_two, key_three = jax.random.split(key, 3)
    fast_share = 0.5
    fast_mask = jax.random.bernoulli(key_one, fast_share, (LRU,))
    slow_rate = jnp.exp(jax.random.uniform(key_two, (LRU,), jnp.float32, math.log(0.03), math.log(0.25))) / TOKENS
    fast_rate = jnp.exp(jax.random.uniform(key_three, (LRU,), jnp.float32, math.log(0.002), math.log(0.008)))
    return jnp.where(fast_mask, fast_rate, slow_rate).astype(jnp.float32)


def with_spikes(entries, own_key, source, target, shards_of, factor):
    owner, partner = [(jnp.arange(entries.shape[axis_at]) // (entries.shape[axis_at] // shards_of)).reshape([-1 if axis == axis_at else 1 for axis in range(entries.ndim)]) for axis_at in (source, target)]
    chosen = jax.random.permutation(own_key, shards_of)[partner]
    strong = (owner == chosen) | (owner == (partner + shards_of // 2) % shards_of)
    return jnp.where(strong, factor * entries, entries)


def steps_of(own_key, extent, cuts, smallest, largest):
    level, own = 1.0, jax.random.fold_in(own_key, 6)
    for position, parts in cuts:
        steps = jnp.exp(jax.random.uniform(jax.random.fold_in(own, position), (parts,), jnp.float32, smallest / len(cuts), largest / len(cuts)))
        level = level * jnp.repeat(steps, extent[position] // parts).reshape([-1 if axis == position else 1 for axis in range(len(extent))])
    return level


def shared_out(rng, own, number, rows, number_of, top, reach, skew):
    order = jax.random.permutation(rng, number_of)
    packed, ordinary = load_shares(number_of, rows * top, reach, skew, True), load_shares(number_of, rows * top, reach, skew, False)
    places = jnp.arange(number_of)

    def named(tallies, turn):
        used = int((tallies > 0).sum())
        fixed = max(1, used // 4)
        moved = fixed + (places - fixed + turn * (used - fixed)) % max(1, number_of - fixed)
        return jnp.zeros((number_of,), jnp.int32).at[order[jnp.where(places < fixed, places, moved)]].set(jnp.asarray(tallies, jnp.int32))

    tallies = jnp.where(number % 4 == 0, named(packed, number // 4), named(ordinary, number - number // 4 - 1))
    mixed = jax.random.permutation(jax.random.fold_in(own, 3), number_of)
    donor, taker = mixed[0:number_of // 2 * 2:2], mixed[1:number_of // 2 * 2:2]
    margin = jnp.minimum(tallies[donor] - 1, reach - tallies[taker]) // 2
    margin = jnp.where((donor == order[0]) | (taker == order[0]) | (tallies[taker] == 0), 0, jnp.maximum(margin, 0))
    moved = jax.random.randint(jax.random.fold_in(own, 4), (number_of // 2,), 0, 1 << 20) % (margin + 1)
    tallies = tallies.at[donor].add(-moved).at[taker].add(moved)
    items = jnp.searchsorted(jnp.cumsum(tallies), jnp.arange(rows * top), side="right").astype(jnp.int32)
    listing = items.reshape(top, rows).T
    listing = listing[jax.random.permutation(jax.random.fold_in(own, 1), rows)]
    turn = jax.random.randint(jax.random.fold_in(own, 2), (rows, 1), 0, top)
    return jnp.take_along_axis(listing, (jnp.arange(top)[None, :] + turn) % top, axis=1)


def load_shares(amount, total, limit, lean, full):
    loads = [(1 << 20) // math.isqrt(standing ** lean) + 1 for standing in range(1, amount + 1)]
    largest = limit if full else min(limit, max(-(-total // amount), total * loads[0] // sum(loads)))
    least = 1 if total - largest >= amount - 1 else 0
    given, rest = [largest] + [least] * (amount - 1), total - largest - least * (amount - 1)
    while rest > 0:
        free = [i for i in range(1, amount) if given[i] < largest] or [i for i in range(1, amount) if given[i] < limit]
        mass, left = sum([loads[i] for i in free]), rest
        for i in free:
            extra = min(limit - given[i], max(1, left * loads[i] // mass), rest)
            given[i] = given[i] + extra
            rest = rest - extra
    return np.array(given)


def scatter_about(stream_key, dims, deviation, reach, cuts=(), held_as=jnp.bfloat16):
    loudness = steps_of(stream_key, dims, cuts, -0.22, 0.18) if cuts else 1.0
    values = jax.random.normal(stream_key, dims, jnp.float32) * deviation * loudness
    return jnp.minimum(jnp.maximum(values, -reach), reach).astype(held_as)


def noise_with(own_key, dims, width, reach, shards, heavy, kind=jnp.bfloat16):
    array = width * jax.random.normal(own_key, dims, jnp.float32)
    if shards:
        array = array * steps_of(own_key, dims, shards, -0.22, 0.18)
    return jnp.clip(with_spikes(array, jax.random.fold_in(own_key, 3), *heavy), -reach, reach).astype(kind)


def setup_inputs(seed: int = 0) -> dict:
    key_list = jax.random.split(jax.random.key(seed), 17)
    cotangent = noise_with(key_list[0], (TOKENS, D), 1.0, 6.0, ((0, 8), (1, 4)), (0, 1, 8, 2.0))
    mixer_out = scatter_about(key_list[1], (TOKENS, D), 1.0, 6.0, ((0, 8), (1, 4)))
    route_ids_keys = jax.random.split(jax.random.fold_in(key_list[2], 1), TOKENS // TOK_DEV)
    route_ids_turns = jax.random.permutation(jax.random.fold_in(key_list[2], 3), TOKENS // TOK_DEV)
    route_ids = jax.vmap(lambda own, number: shared_out(jax.random.fold_in(key_list[2], 2), own, number, TOK_DEV, EXPERTS, 2, CAP, 2))(route_ids_keys, route_ids_turns).reshape((TOKENS, 2))
    route_weights = jnp.clip(0.2 + 0.8 * jax.random.uniform(key_list[3], (TOKENS, 2), jnp.float32) ** steps_of(key_list[3], (TOKENS, 2), ((0, 8),), -0.2, 0.2), 0.2, 1.0)
    conv_out = scatter_about(key_list[4], (TOKENS, LRU), 1.0, 6.0, ((0, 8), (1, 4)))
    recur_gate = draw_recur_gate(jax.random.fold_in(key_list[16], 71), 0)
    input_gate = jnp.clip(0.099609375 + 0.7988281 * jax.random.uniform(key_list[6], (TOKENS, LRU), jnp.float32) ** steps_of(key_list[6], (TOKENS, LRU), ((0, 8), (1, 4)), -0.2, 0.2), 0.099609375, 0.8984375).astype(jnp.bfloat16)
    gate_pre = scatter_about(key_list[7], (TOKENS, LRU), 1.0, 6.0, ((0, 8), (1, 4)))
    states_before = scatter_about(key_list[8], (TOKENS, LRU), 0.5, 4.0, ((0, 8), (1, 4)))
    decay_rate = draw_decay_rate(jax.random.fold_in(key_list[16], 71), 0)
    out_proj = scatter_about(key_list[10], (D, LRU), LRU ** -0.5, 0.125, ((1, 4),))
    recur_map = scatter_about(key_list[11], (BLOCKS, BLOCK_W, BLOCK_W), BLOCK_W ** -0.5, 0.25, ((0, 4),))
    input_map = scatter_about(key_list[12], (BLOCKS, BLOCK_W, BLOCK_W), BLOCK_W ** -0.5, 0.25, ((0, 4),))
    expert_gate = scatter_about(key_list[13], (EXPERTS, D, FF), D ** -0.5, 0.125, ((0, 8), (2, 4)))
    expert_up = scatter_about(key_list[14], (EXPERTS, D, FF), D ** -0.5, 0.125, ((0, 8), (2, 4)))
    expert_down = scatter_about(key_list[15], (EXPERTS, FF, D), FF ** -0.5, 0.1875, ((0, 8), (1, 4)))
    return dict(cotangent=cotangent, mixer_out=mixer_out, route_ids=route_ids, route_weights=route_weights, conv_out=conv_out, recur_gate=recur_gate, input_gate=input_gate, gate_pre=gate_pre, states_before=states_before, decay_rate=decay_rate, out_proj=out_proj, recur_map=recur_map, input_map=input_map, expert_gate=expert_gate, expert_up=expert_up, expert_down=expert_down)


def silu_parts(values):
    sig = jax.nn.sigmoid(values)
    return (values * sig, sig * (1.0 + values * (1.0 - sig)))

def route_slots(route_block):
    flat_ids = route_block.reshape(-1)
    onehot = (flat_ids[:, None] == jnp.arange(EXPERTS, dtype=jnp.int32)[None, :]).astype(jnp.int32)
    before = jnp.cumsum(onehot, axis=0) - onehot
    slot_rank = lax.optimization_barrier(jnp.sum(before * onehot, axis=1))
    return (flat_ids * CAP + slot_rank).astype(jnp.int32)

def link_steps(earlier, later):
    return (earlier[0] * later[0], later[0] * earlier[1] + later[1])

def reference(cotangent, mixer_out, route_ids, route_weights, conv_out, recur_gate, input_gate, gate_pre, states_before, decay_rate, out_proj, recur_map, input_map, expert_gate, expert_up, expert_down):
    slot_pos = jax.vmap(route_slots)(route_ids.reshape(N_SP, TOK_DEV, 2))
    expert_of = slot_pos // CAP
    slot_rank = slot_pos % CAP
    source = jnp.arange(N_SP, dtype=jnp.int32)[:, None]
    place = (expert_of * (N_SP * CAP) + source * CAP + slot_rank).astype(jnp.int32).reshape(-1)
    token_of = (source * TOK_DEV + jnp.arange(2 * TOK_DEV, dtype=jnp.int32)[None, :] // 2).astype(jnp.int32)
    table = jnp.full((EXPERTS * N_SP * CAP,), TOKENS, jnp.int32).at[place].set(token_of.reshape(-1))
    slot_weight = jnp.zeros((EXPERTS * N_SP * CAP,), jnp.float32).at[place].set(route_weights.astype(jnp.float32).reshape(-1))
    table = table.reshape(EXPERTS, N_SP * CAP)
    slot_weight = slot_weight.reshape(EXPERTS, N_SP * CAP)
    x_padded = jnp.concatenate([mixer_out, jnp.zeros((1, D), jnp.bfloat16)], axis=0)
    g_padded = jnp.concatenate([cotangent, jnp.zeros((1, D), jnp.bfloat16)], axis=0)

    def expert_step(routed_sum, inputs):
        row_index, weight, w_gate, w_up, w_down = inputs
        row_data = x_padded[row_index]
        routed_cot = (g_padded[row_index].astype(jnp.float32) * weight[:, None]).astype(jnp.bfloat16)
        pre_gate = jnp.dot(row_data, w_gate, preferred_element_type=jnp.float32)
        pre_up = jnp.dot(row_data, w_up, preferred_element_type=jnp.float32)
        gate_act, slope = silu_parts(pre_gate)
        active = (gate_act * pre_up).astype(jnp.bfloat16)
        d_active = jnp.dot(routed_cot, w_down.T, preferred_element_type=jnp.float32)
        grad_down = jnp.dot(active.T, routed_cot, preferred_element_type=jnp.float32).astype(jnp.bfloat16)
        d_gate = (d_active * pre_up * slope).astype(jnp.bfloat16)
        d_up = (d_active * gate_act).astype(jnp.bfloat16)
        grad_gate = jnp.dot(row_data.T, d_gate, preferred_element_type=jnp.float32).astype(jnp.bfloat16)
        grad_up = jnp.dot(row_data.T, d_up, preferred_element_type=jnp.float32).astype(jnp.bfloat16)
        route_grad = (jnp.dot(d_gate, w_gate.T, preferred_element_type=jnp.float32) + jnp.dot(d_up, w_up.T, preferred_element_type=jnp.float32)).astype(jnp.bfloat16)
        routed_sum = routed_sum.at[row_index].add(route_grad.astype(jnp.float32))
        return (routed_sum, (grad_gate, grad_up, grad_down))
    routed_sum, expert_grads = lax.scan(expert_step, jnp.zeros((TOKENS + 1, D), jnp.float32), (table, slot_weight, expert_gate, expert_up, expert_down))
    grad_expert_gate, grad_expert_up, grad_expert_down = expert_grads
    out_grad = (cotangent.astype(jnp.float32) + routed_sum[:TOKENS]).astype(jnp.bfloat16)
    rate = decay_rate.astype(jnp.float32)[None, :]
    recur_f = recur_gate.astype(jnp.float32)
    input_f = input_gate.astype(jnp.float32)
    conv_f = conv_out.astype(jnp.float32)
    before_f = states_before.astype(jnp.float32)
    log_decay = -8.0 * recur_f * rate
    decay_now = jnp.exp(log_decay)
    at_start = (jnp.arange(TOKENS, dtype=jnp.int32) == 0)[:, None]
    norm_factor = jnp.where(at_start, 1.0, jnp.sqrt(-jnp.expm1(2.0 * log_decay)))
    norm_slope = jnp.where(at_start, 0.0, -jnp.exp(2.0 * log_decay) / norm_factor)
    drive = input_f * conv_f
    state = decay_now * before_f + norm_factor * drive
    gate, gelu_back = jax.vjp(jax.nn.gelu, gate_pre.astype(jnp.float32))
    mixed = (state * gate).astype(jnp.bfloat16)
    d_mixed = jnp.dot(out_grad, out_proj, preferred_element_type=jnp.float32)
    grad_out_proj = jnp.dot(out_grad.T, mixed, preferred_element_type=jnp.float32)
    grad_gate_pre = gelu_back(d_mixed * state)[0].astype(jnp.bfloat16)
    decay_next = jnp.concatenate([decay_now[1:], jnp.ones((1, LRU), jnp.float32)], axis=0)
    _, state_grad = lax.associative_scan(link_steps, (decay_next, d_mixed * gate), axis=0, reverse=True)
    d_log = state_grad * (decay_now * before_f + norm_slope * drive)
    d_recur_pre = (d_log * (-8.0 * rate) * recur_f * (1.0 - recur_f)).astype(jnp.bfloat16)
    d_input_pre = (state_grad * norm_factor * conv_f * input_f * (1.0 - input_f)).astype(jnp.bfloat16)
    through_recur = jnp.einsum('tbj,bij->tbi', d_recur_pre.astype(jnp.float32).reshape(TOKENS, BLOCKS, BLOCK_W), recur_map.astype(jnp.float32))
    through_input = jnp.einsum('tbj,bij->tbi', d_input_pre.astype(jnp.float32).reshape(TOKENS, BLOCKS, BLOCK_W), input_map.astype(jnp.float32))
    grad_conv = (state_grad * norm_factor * input_f + (through_recur + through_input).reshape(TOKENS, LRU)).astype(jnp.bfloat16)
    return (grad_expert_gate, grad_expert_up, grad_expert_down, grad_out_proj, grad_conv, grad_gate_pre)
```

```python
import functools

import jax
import jax.numpy as jnp
from jax import lax
from jax.experimental import pallas as pl
from jax.experimental.pallas import tpu as pltpu
from jax.sharding import PartitionSpec as P

MESH = pl.DeviceIdType.MESH
VMEM = pl.BlockSpec(memory_space=pltpu.VMEM)
DMA = pltpu.SemaphoreType.DMA


def bits_of(count):
    found, bit = [], 1
    while bit < count:
        found.insert(0, bit)
        bit *= 2
    return found


def low_bit(mask):
    return mask & -mask


def flip(index, mask):
    bit = 1
    while bit <= mask:
        if mask & bit:
            index = index + bit - 2 * bit * lax.rem(lax.div(index, bit), 2)
        bit *= 2
    return index


def window(index, width):
    return pl.ds(pl.multiple_of(index * width, width), width)


def remote(source, target, send_sem, recv_sem, device):
    return pltpu.make_async_remote_copy(
        src_ref=source,
        dst_ref=target,
        send_sem=send_sem,
        recv_sem=recv_sem,
        device_id=device,
        device_id_type=MESH,
    )


def greet(peers):
    barrier = pltpu.get_barrier_semaphore()
    for peer in peers:
        pl.semaphore_signal(barrier, inc=1, device_id=peer, device_id_type=MESH)
    pl.semaphore_wait(barrier, len(peers))


def relays_of(count):
    masks = [mask for mask in range(1, count) if mask != low_bit(mask)]
    return sorted(masks, key=lambda mask: (bin(mask).count("1"), -mask))


def call(kernel, out_shape, scratch, ident, *operands):
    return pl.pallas_call(
        kernel,
        out_shape=out_shape,
        in_specs=[VMEM] * len(operands),
        out_specs=jax.tree.map(lambda _: VMEM, out_shape),
        scratch_shapes=scratch,
        compiler_params=pltpu.CompilerParams(
            collective_id=ident, has_side_effects=True, vmem_limit_bytes=48 * 1024 * 1024
        ),
    )(*operands)


def dispatch_kernel(n_sp, n_tp, rows, cots, got_rows, got_cots, own_sem, sa, ra, st, rt):
    s, t = lax.axis_index("sp"), lax.axis_index("tp")
    width = rows.shape[-1]
    kinds = ((rows, got_rows), (cots, got_cots))
    greet(
        [(flip(s, m), t) for m in range(1, n_sp)] + [(s, flip(t, b)) for b in bits_of(n_tp)]
    )

    def own(kind):
        source, target = kinds[kind]
        return pltpu.make_async_copy(
            source.at[s], target.at[s, :, window(t, width)], own_sem.at[kind]
        )

    def to_expert(kind, m):
        source, target = kinds[kind]
        q = flip(s, m)
        return remote(
            source.at[q], target.at[s, :, window(t, width)], sa.at[kind, m], ra.at[kind, m], (q, t)
        )

    def share(kind, m, k):
        bit = low_bit(k)
        block = kinds[kind][1].at[flip(s, m), :, window(flip(t, k - bit), width)]
        return remote(block, block, st.at[kind, m, k], rt.at[kind, m, k], (s, flip(t, bit)))

    seen = set()

    def forward(m):
        for kind in range(2):
            for k in relays_of(n_tp):
                before = k - low_bit(k)
                if (kind, m, before) not in seen:
                    share(kind, m, before).wait_recv()
                    seen.add((kind, m, before))
                share(kind, m, k).start()

    for kind in range(2):
        own(kind).start()
    for m in range(1, n_sp):
        for kind in range(2):
            to_expert(kind, m).start()
    for m in range(n_sp):
        for kind in range(2):
            if m == 0:
                own(kind).wait()
            else:
                to_expert(kind, m).wait_recv()
            for bit in bits_of(n_tp):
                share(kind, m, bit).start()
        if m > 0:
            forward(m - 1)
    forward(n_sp - 1)
    for kind in range(2):
        for m in range(n_sp):
            if m > 0:
                to_expert(kind, m).wait_send()
            for k in range(1, n_tp):
                share(kind, m, k).wait_send()
                if (kind, m, k) not in seen:
                    share(kind, m, k).wait_recv()


def combine_kernel(
    n_sp, n_tp, part, mixed, ret, mixed_all, half, xsend, xrecv, back,
    own_sem, sh, rh, sx, rx, sb, rb, sg, rg,
):
    s, t = lax.axis_index("sp"), lax.axis_index("tp")
    width = ret.shape[-1]
    pair, across = flip(t, 1), flip(t, 2)
    greet(
        [(flip(s, m), t) for m in range(1, n_sp)] + [(s, flip(t, b)) for b in bits_of(n_tp)]
    )

    def to_pair(slot):
        chunk = flip(pair, 2) if slot == 0 else pair
        return remote(
            part.at[:, :, window(chunk, width)], half.at[slot], sh.at[slot], rh.at[slot], (s, pair)
        )

    def cross(m):
        q = flip(s, m)
        return remote(xsend.at[q], xrecv.at[q], sx.at[m], rx.at[m], (s, across))

    def give(m):
        q = flip(s, m)
        return remote(back.at[q], ret.at[s], sb.at[m], rb.at[m], (q, t))

    def gather(k):
        bit = low_bit(k)
        block = flip(s, k - bit)
        source = mixed if k == bit else mixed_all.at[block]
        return remote(source, mixed_all.at[block], sg.at[k], rg.at[k], (flip(s, bit), t))

    seen = set()

    def forward(masks):
        for k in masks:
            before = k - low_bit(k)
            if before not in seen:
                gather(before).wait_recv()
                seen.add(before)
            gather(k).start()

    to_pair(0).start()
    to_pair(1).start()
    own = pltpu.make_async_copy(mixed, mixed_all.at[s], own_sem)
    own.start()
    for bit in bits_of(n_sp):
        gather(bit).start()
    order = list(range(1, n_sp)) + [0]
    to_pair(0).wait_recv()
    for m in order:
        q = flip(s, m)
        xsend[q] = (
            part[q, :, window(across, width)].astype(jnp.float32) + half[0, q].astype(jnp.float32)
        ).astype(jnp.bfloat16)
        cross(m).start()
    to_pair(1).wait_recv()
    relays = relays_of(n_sp)
    early = [k for k in relays if k - low_bit(k) == n_sp // 2]
    for place, m in enumerate(order):
        q = flip(s, m)
        cross(m).wait_recv()
        total = (
            part[q, :, window(t, width)].astype(jnp.float32)
            + half[1, q].astype(jnp.float32)
            + xrecv[q].astype(jnp.float32)
        ).astype(jnp.bfloat16)
        if m == 0:
            ret[s] = total
        else:
            back[q] = total
            give(m).start()
        if place == n_sp // 2 - 1:
            forward(early)
    forward([k for k in relays if k not in early])
    own.wait()
    for slot in range(2):
        to_pair(slot).wait_send()
    for m in range(n_sp):
        cross(m).wait_send()
        if m > 0:
            give(m).wait_send()
            give(m).wait_recv()
            gather(m).wait_send()
            if m not in seen:
                gather(m).wait_recv()


def widen_kernel(n_tp, part, out, own_sem, st, rt):
    s, t = lax.axis_index("sp"), lax.axis_index("tp")
    width = part.shape[-1]
    greet([(s, flip(t, b)) for b in bits_of(n_tp)])

    def share(k):
        bit = low_bit(k)
        block = out.at[:, window(flip(t, k - bit), width)]
        source = part if k == bit else block
        return remote(source, block, st.at[k], rt.at[k], (s, flip(t, bit)))

    for bit in bits_of(n_tp):
        share(bit).start()
    own = pltpu.make_async_copy(part, out.at[:, window(t, width)], own_sem)
    own.start()
    seen = set()
    for k in relays_of(n_tp):
        before = k - low_bit(k)
        if before not in seen:
            share(before).wait_recv()
            seen.add(before)
        share(k).start()
    own.wait()
    for k in range(1, n_tp):
        share(k).wait_send()
        if k not in seen:
            share(k).wait_recv()


def scan_kernel(
    n_sp, flipped, drive, decay, state_grad, pieces, weight, carry, carries,
    own_sem, sa, ra, sc, rc,
):
    s, t = lax.axis_index("sp"), lax.axis_index("tp")
    rows = drive.shape[0]
    share = flipped.shape[0] // n_sp
    greet([(flip(s, m), t) for m in range(1, n_sp)])

    def piece(m):
        q = flip(s, m)
        return remote(
            flipped.at[window(q, share)], pieces.at[:, window(s, rows)], sa.at[m], ra.at[m], (q, t)
        )

    def send_carry(m):
        return remote(carry, carries.at[s], sc.at[m], rc.at[m], (flip(s, m), t))

    own = pltpu.make_async_copy(
        flipped.at[window(s, share)], pieces.at[:, window(s, rows)], own_sem
    )
    own.start()

    def lap(step, held):
        grad, product = held
        row = rows - 1 - step
        grad = drive[pl.ds(row, 1), :] + grad
        product_here = product
        state_grad[pl.ds(row, 1), :] = grad
        weight[pl.ds(row, 1), :] = product_here
        now = decay[pl.ds(row, 1), :]
        return (now * grad, now * product_here)

    zero = jnp.zeros((1, drive.shape[1]), jnp.float32)
    start, span = lax.fori_loop(0, rows, lap, (zero, zero + 1.0), unroll=8)
    carry[0:1, :] = span
    carry[1:2, :] = start
    for m in range(1, n_sp):
        send_carry(m).start()
    for m in range(1, n_sp):
        piece(m).start()
    for m in range(1, n_sp):
        send_carry(m).wait_recv()
    incoming = zero
    for later in range(n_sp - 1, 0, -1):
        longer = carries[later, 1:2, :] + carries[later, 0:1, :] * incoming
        incoming = jnp.where(later > s, longer, incoming)
    state_grad[...] = state_grad[...] + weight[...] * incoming
    own.wait()
    for m in range(1, n_sp):
        send_carry(m).wait_send()
        piece(m).wait_send()
        piece(m).wait_recv()


def silu_parts(values):
    sig = jax.nn.sigmoid(values)
    return (values * sig, sig * (1.0 + values * (1.0 - sig)))


def route_slots(route_block, experts, capacity):
    flat_ids = route_block.reshape(-1)
    onehot = (flat_ids[:, None] == jnp.arange(experts, dtype=jnp.int32)[None, :]).astype(jnp.int32)
    before = jnp.cumsum(onehot, axis=0) - onehot
    slot_rank = jnp.sum(before * onehot, axis=1)
    return flat_ids * capacity + slot_rank


def contract_rows(left, right):
    return lax.dot_general(
        left, right, (((0,), (0,)), ((), ())), preferred_element_type=jnp.float32
    )


def body(
    cotangent,
    mixer_out,
    route_ids,
    route_weights,
    conv_out,
    recur_gate,
    input_gate,
    gate_pre,
    states_before,
    decay_rate,
    out_proj,
    recur_map,
    input_map,
    expert_gate,
    expert_up,
    expert_down,
):
    row_count = cotangent.shape[0]
    experts = lax.axis_size("sp")
    capacity = 4 * row_count // experts
    slot_pos = route_slots(route_ids, experts, capacity).reshape(row_count, 2)
    slot_range = jnp.arange(experts * capacity, dtype=jnp.int32)[:, None]
    hit_first = slot_range == slot_pos[None, :, 0]
    hit_second = slot_range == slot_pos[None, :, 1]
    dispatch = (hit_first | hit_second).astype(jnp.bfloat16)
    slot_weight = jnp.sum(
        jnp.where(hit_first, route_weights[None, :, 0], 0.0)
        + jnp.where(hit_second, route_weights[None, :, 1], 0.0),
        axis=1,
    )
    send_rows = jnp.dot(dispatch, mixer_out, preferred_element_type=jnp.float32).astype(
        jnp.bfloat16
    )
    send_cot = (
        jnp.dot(dispatch, cotangent, preferred_element_type=jnp.float32) * slot_weight[:, None]
    ).astype(jnp.bfloat16)
    tps = lax.axis_size("tp")
    features = tps * cotangent.shape[1]
    slots = experts * capacity
    blocks = (experts, capacity, features)
    got_rows, got_cot = call(
        functools.partial(dispatch_kernel, experts, tps),
        [jax.ShapeDtypeStruct(blocks, jnp.bfloat16)] * 2,
        [
            DMA((2,)),
            DMA((2, experts)),
            DMA((2, experts)),
            DMA((2, experts, tps)),
            DMA((2, experts, tps)),
        ],
        0,
        send_rows.reshape(experts, capacity, -1),
        send_cot.reshape(experts, capacity, -1),
    )
    got_rows, got_cot = (got_rows.reshape(slots, features), got_cot.reshape(slots, features))
    w_gate = expert_gate[0]
    w_up = expert_up[0]
    w_down = expert_down[0]
    pre_gate = jnp.dot(got_rows, w_gate, preferred_element_type=jnp.float32)
    pre_up = jnp.dot(got_rows, w_up, preferred_element_type=jnp.float32)
    gate_act, slope = silu_parts(pre_gate)
    active = (gate_act * pre_up).astype(jnp.bfloat16)
    d_active = lax.dot_general(
        got_cot, w_down, (((1,), (1,)), ((), ())), preferred_element_type=jnp.float32
    )
    grad_down = contract_rows(active, got_cot).astype(jnp.bfloat16)
    d_gate = (d_active * pre_up * slope).astype(jnp.bfloat16)
    d_up = (d_active * gate_act).astype(jnp.bfloat16)
    grad_gate = contract_rows(got_rows, d_gate).astype(jnp.bfloat16)
    grad_up = contract_rows(got_rows, d_up).astype(jnp.bfloat16)
    partial_grad = lax.dot_general(
        d_gate, w_gate, (((1,), (1,)), ((), ())), preferred_element_type=jnp.float32
    ) + lax.dot_general(d_up, w_up, (((1,), (1,)), ((), ())), preferred_element_type=jnp.float32)
    channels = conv_out.shape[1]
    rate = decay_rate[None, :]
    recur_f = recur_gate.astype(jnp.float32)
    input_f = input_gate.astype(jnp.float32)
    conv_f = conv_out.astype(jnp.float32)
    before_f = states_before.astype(jnp.float32)
    log_decay = -8.0 * recur_f * rate
    decay_now = jnp.exp(log_decay)
    position = lax.axis_index("sp") * row_count + jnp.arange(row_count, dtype=jnp.int32)
    at_start = (position == 0)[:, None]
    norm_factor = jnp.where(at_start, 1.0, jnp.sqrt(-jnp.expm1(2.0 * log_decay)))
    norm_slope = jnp.where(at_start, 0.0, -jnp.exp(2.0 * log_decay) / norm_factor)
    drive = input_f * conv_f
    state = decay_now * before_f + norm_factor * drive
    gate, gelu_back = jax.vjp(jax.nn.gelu, gate_pre.astype(jnp.float32))
    mixed = (state * gate).astype(jnp.bfloat16)
    block = (experts, capacity, cotangent.shape[1])
    pair_sems, own_sems = (DMA((2,)), DMA((experts,)))
    returned, mixed_all = call(
        functools.partial(combine_kernel, experts, tps),
        [
            jax.ShapeDtypeStruct(block, jnp.bfloat16),
            jax.ShapeDtypeStruct((experts, row_count, channels), jnp.bfloat16),
        ],
        [
            pltpu.VMEM((2, *block), jnp.bfloat16),
            pltpu.VMEM(block, jnp.bfloat16),
            pltpu.VMEM(block, jnp.bfloat16),
            pltpu.VMEM(block, jnp.bfloat16),
            DMA,
            pair_sems,
            pair_sems,
            *([own_sems] * 6),
        ],
        1,
        partial_grad.astype(jnp.bfloat16).reshape(blocks),
        mixed,
    )
    returned = returned.reshape(slots, -1)
    grad_part = (cotangent.astype(jnp.float32) + contract_rows(dispatch, returned)).astype(
        jnp.bfloat16
    )
    out_grad = call(
        functools.partial(widen_kernel, tps),
        jax.ShapeDtypeStruct((row_count, features), jnp.bfloat16),
        [DMA, DMA((tps,)), DMA((tps,))],
        2,
        grad_part,
    )
    d_mixed = jnp.dot(out_grad, out_proj, preferred_element_type=jnp.float32)
    state_grad, pieces = call(
        functools.partial(scan_kernel, experts),
        [
            jax.ShapeDtypeStruct((row_count, channels), jnp.float32),
            jax.ShapeDtypeStruct((features // experts, experts * row_count), jnp.bfloat16),
        ],
        [
            pltpu.VMEM((row_count, channels), jnp.float32),
            pltpu.VMEM((2, channels), jnp.float32),
            pltpu.VMEM((experts, 2, channels), jnp.float32),
            DMA,
            *([own_sems] * 4),
        ],
        3,
        out_grad.T,
        d_mixed * gate,
        decay_now,
    )
    grad_out_proj = jnp.dot(
        pieces,
        mixed_all.reshape(experts * row_count, channels),
        preferred_element_type=jnp.float32,
    )
    grad_gate_pre = gelu_back(d_mixed * state)[0].astype(jnp.bfloat16)
    d_log = state_grad * (decay_now * before_f + norm_slope * drive)
    d_recur_pre = (d_log * (-8.0 * rate) * recur_f * (1.0 - recur_f)).astype(jnp.bfloat16)
    d_input_pre = (state_grad * norm_factor * conv_f * input_f * (1.0 - input_f)).astype(
        jnp.bfloat16
    )
    groups = recur_map.shape[0]
    width = recur_map.shape[1]
    through_recur = jnp.einsum(
        "tbj,bij->tbi",
        d_recur_pre.reshape(row_count, groups, width),
        recur_map,
        preferred_element_type=jnp.float32,
    )
    through_input = jnp.einsum(
        "tbj,bij->tbi",
        d_input_pre.reshape(row_count, groups, width),
        input_map,
        preferred_element_type=jnp.float32,
    )
    grad_conv = (
        state_grad * norm_factor * input_f
        + (through_recur + through_input).reshape(row_count, channels)
    ).astype(jnp.bfloat16)
    return (
        grad_gate[None],
        grad_up[None],
        grad_down[None],
        grad_out_proj,
        grad_conv,
        grad_gate_pre,
    )


def solution(mesh):
    placed = (
        P("sp", "tp"),
        P("sp", "tp"),
        P("sp", None),
        P("sp", None),
        P("sp", "tp"),
        P("sp", "tp"),
        P("sp", "tp"),
        P("sp", "tp"),
        P("sp", "tp"),
        P("tp"),
        P(None, "tp"),
        P("tp", None, None),
        P("tp", None, None),
        P("sp", None, "tp"),
        P("sp", None, "tp"),
        P("sp", "tp", None),
    )
    return jax.shard_map(
        body,
        mesh=mesh,
        in_specs=placed,
        out_specs=(
            P("sp", None, "tp"),
            P("sp", None, "tp"),
            P("sp", "tp", None),
            P("sp", "tp"),
            P("sp", "tp"),
            P("sp", "tp"),
        ),
        check_vma=False,
    )
```

```python
import functools

import jax
import jax.numpy as jnp
from jax import lax
from jax.experimental import pallas as pl
from jax.experimental.pallas import tpu as pltpu
from jax.sharding import PartitionSpec as P

MESH = pl.DeviceIdType.MESH
VMEM = pl.BlockSpec(memory_space=pltpu.VMEM)
DMA = pltpu.SemaphoreType.DMA


def bits_of(count):
    found, bit = [], 1
    while bit < count:
        found.insert(0, bit)
        bit *= 2
    return found


def low_bit(mask):
    return mask & -mask


def flip(index, mask):
    bit = 1
    while bit <= mask:
        if mask & bit:
            index = index + bit - 2 * bit * lax.rem(lax.div(index, bit), 2)
        bit *= 2
    return index


def window(index, width):
    return pl.ds(pl.multiple_of(index * width, width), width)


def remote(source, target, send_sem, recv_sem, device):
    return pltpu.make_async_remote_copy(
        src_ref=source,
        dst_ref=target,
        send_sem=send_sem,
        recv_sem=recv_sem,
        device_id=device,
        device_id_type=MESH,
    )


def greet(peers):
    barrier = pltpu.get_barrier_semaphore()
    for peer in peers:
        pl.semaphore_signal(barrier, inc=1, device_id=peer, device_id_type=MESH)
    pl.semaphore_wait(barrier, len(peers))


def relays_of(count):
    masks = [mask for mask in range(1, count) if mask != low_bit(mask)]
    return sorted(masks, key=lambda mask: (bin(mask).count("1"), -mask))


def call(kernel, out_shape, scratch, ident, *operands):
    return pl.pallas_call(
        kernel,
        out_shape=out_shape,
        in_specs=[VMEM] * len(operands),
        out_specs=jax.tree.map(lambda _: VMEM, out_shape),
        scratch_shapes=scratch,
        compiler_params=pltpu.CompilerParams(
            collective_id=ident, has_side_effects=True, vmem_limit_bytes=48 * 1024 * 1024
        ),
    )(*operands)


def dispatch_kernel(n_sp, n_tp, rows, cots, got_rows, got_cots, own_sem, sa, ra, st, rt):
    s, t = lax.axis_index("sp"), lax.axis_index("tp")
    width = rows.shape[-1]
    kinds = ((rows, got_rows), (cots, got_cots))
    greet(
        [(flip(s, m), t) for m in range(1, n_sp)] + [(s, flip(t, b)) for b in bits_of(n_tp)]
    )

    def own(kind):
        source, target = kinds[kind]
        return pltpu.make_async_copy(
            source.at[s], target.at[s, :, window(t, width)], own_sem.at[kind]
        )

    def to_expert(kind, m):
        source, target = kinds[kind]
        q = flip(s, m)
        return remote(
            source.at[q], target.at[s, :, window(t, width)], sa.at[kind, m], ra.at[kind, m], (q, t)
        )

    def share(kind, m, k):
        bit = low_bit(k)
        block = kinds[kind][1].at[flip(s, m), :, window(flip(t, k - bit), width)]
        return remote(block, block, st.at[kind, m, k], rt.at[kind, m, k], (s, flip(t, bit)))

    seen = set()

    def forward(m):
        for kind in range(2):
            for k in relays_of(n_tp):
                before = k - low_bit(k)
                if (kind, m, before) not in seen:
                    share(kind, m, before).wait_recv()
                    seen.add((kind, m, before))
                share(kind, m, k).start()

    for kind in range(2):
        own(kind).start()
    far, near = list(range(n_sp - 1, n_sp // 2 - 1, -1)), list(range(n_sp // 2 - 1, 1, -1))
    for m in [1] + far + near:
        for kind in range(2):
            to_expert(kind, m).start()
    half = len(far) // 2
    arrivals = [0, 1] + far[:half] + near + far[half:]
    for place, m in enumerate(arrivals):
        for kind in range(2):
            if m == 0:
                own(kind).wait()
            else:
                to_expert(kind, m).wait_recv()
            for bit in bits_of(n_tp):
                share(kind, m, bit).start()
        if place > 0:
            forward(arrivals[place - 1])
    forward(arrivals[-1])
    for kind in range(2):
        for m in range(n_sp):
            if m > 0:
                to_expert(kind, m).wait_send()
            for k in range(1, n_tp):
                share(kind, m, k).wait_send()
                if (kind, m, k) not in seen:
                    share(kind, m, k).wait_recv()


def combine_kernel(
    n_sp, n_tp, part, mixed, base, pick, out, mixed_all, half, xsend, xrecv, back, ret,
    own_sem, sh, rh, sx, rx, sb, rb, sg, rg, st, rt,
):
    s, t = lax.axis_index("sp"), lax.axis_index("tp")
    width = ret.shape[-1]
    pair, across = flip(t, 1), flip(t, 2)
    greet(
        [(flip(s, m), t) for m in range(1, n_sp)] + [(s, flip(t, b)) for b in bits_of(n_tp)]
    )

    def to_pair(slot):
        chunk = flip(pair, 2) if slot == 0 else pair
        return remote(
            part.at[:, :, window(chunk, width)], half.at[slot], sh.at[slot], rh.at[slot], (s, pair)
        )

    def cross(m):
        q = flip(s, m)
        return remote(xsend.at[q], xrecv.at[q], sx.at[m], rx.at[m], (s, across))

    def give(m):
        q = flip(s, m)
        return remote(back.at[q], ret.at[s], sb.at[m], rb.at[m], (q, t))

    def gather(k):
        bit = low_bit(k)
        block = flip(s, k - bit)
        source = mixed if k == bit else mixed_all.at[block]
        return remote(source, mixed_all.at[block], sg.at[k], rg.at[k], (flip(s, bit), t))

    seen = set()

    def forward(masks):
        for k in masks:
            before = k - low_bit(k)
            if before not in seen:
                gather(before).wait_recv()
                seen.add(before)
            gather(k).start()

    to_pair(0).start()
    to_pair(1).start()
    own = pltpu.make_async_copy(mixed, mixed_all.at[s], own_sem)
    own.start()
    for bit in bits_of(n_sp):
        gather(bit).start()
    order = list(range(n_sp - 1, -1, -1))
    to_pair(0).wait_recv()
    for m in order:
        q = flip(s, m)
        xsend[q] = (
            part[q, :, window(across, width)].astype(jnp.float32) + half[0, q].astype(jnp.float32)
        ).astype(jnp.bfloat16)
        cross(m).start()
    to_pair(1).wait_recv()
    relays = relays_of(n_sp)
    early = [k for k in relays if bin(k).count("1") == 2]
    forward(early)
    for place, m in enumerate(order):
        q = flip(s, m)
        cross(m).wait_recv()
        total = (
            part[q, :, window(t, width)].astype(jnp.float32)
            + half[1, q].astype(jnp.float32)
            + xrecv[q].astype(jnp.float32)
        ).astype(jnp.bfloat16)
        if m == 0:
            ret[s] = total
        else:
            back[q] = total
            give(m).start()
        if place == n_sp // 2:
            forward([k for k in relays if k not in early])
    total = base[...].astype(jnp.float32)
    for m in range(n_sp):
        q = flip(s, m)
        if m > 0:
            give(m).wait_recv()
        total = total + contract_rows(pick[q], ret[q])
    out[:, window(t, width)] = total.astype(jnp.bfloat16)

    def share(k):
        bit = low_bit(k)
        block = out.at[:, window(flip(t, k - bit), width)]
        return remote(block, block, st.at[k], rt.at[k], (s, flip(t, bit)))

    for bit in bits_of(n_tp):
        share(bit).start()
    shared = set()
    for k in relays_of(n_tp):
        before = k - low_bit(k)
        if before not in shared:
            share(before).wait_recv()
            shared.add(before)
        share(k).start()
    for k in range(1, n_tp):
        share(k).wait_send()
        if k not in shared:
            share(k).wait_recv()
    own.wait()
    for slot in range(2):
        to_pair(slot).wait_send()
    for m in range(n_sp):
        cross(m).wait_send()
        if m > 0:
            give(m).wait_send()
            gather(m).wait_send()
            if m not in seen:
                gather(m).wait_recv()


def scan_kernel(
    n_sp, flipped, drive, decay, state_grad, pieces, weight, carry, carries,
    own_sem, sa, ra, sc, rc,
):
    s, t = lax.axis_index("sp"), lax.axis_index("tp")
    rows = drive.shape[0]
    share = flipped.shape[0] // n_sp
    greet([(flip(s, m), t) for m in range(1, n_sp)])

    def piece(m):
        q = flip(s, m)
        return remote(
            flipped.at[window(q, share)], pieces.at[:, window(s, rows)], sa.at[m], ra.at[m], (q, t)
        )

    def send_carry(m):
        return remote(carry, carries.at[s], sc.at[m], rc.at[m], (flip(s, m), t))

    own = pltpu.make_async_copy(
        flipped.at[window(s, share)], pieces.at[:, window(s, rows)], own_sem
    )
    own.start()

    def lap(step, held):
        grad, product = held
        row = rows - 1 - step
        grad = drive[pl.ds(row, 1), :] + grad
        product_here = product
        state_grad[pl.ds(row, 1), :] = grad
        weight[pl.ds(row, 1), :] = product_here
        now = decay[pl.ds(row, 1), :]
        return (now * grad, now * product_here)

    zero = jnp.zeros((1, drive.shape[1]), jnp.float32)
    start, span = lax.fori_loop(0, rows, lap, (zero, zero + 1.0), unroll=8)
    carry[0:1, :] = span
    carry[1:2, :] = start
    for m in range(1, n_sp):
        send_carry(m).start()
    for m in range(1, n_sp):
        piece(m).start()
    for m in range(1, n_sp):
        send_carry(m).wait_recv()
    incoming = zero
    for later in range(n_sp - 1, 0, -1):
        longer = carries[later, 1:2, :] + carries[later, 0:1, :] * incoming
        incoming = jnp.where(later > s, longer, incoming)
    state_grad[...] = state_grad[...] + weight[...] * incoming
    own.wait()
    for m in range(1, n_sp):
        send_carry(m).wait_send()
        piece(m).wait_send()
        piece(m).wait_recv()


def silu_parts(values):
    sig = jax.nn.sigmoid(values)
    return (values * sig, sig * (1.0 + values * (1.0 - sig)))


def route_slots(route_block, experts, capacity):
    flat_ids = route_block.reshape(-1)
    onehot = (flat_ids[:, None] == jnp.arange(experts, dtype=jnp.int32)[None, :]).astype(jnp.int32)
    before = jnp.cumsum(onehot, axis=0) - onehot
    slot_rank = jnp.sum(before * onehot, axis=1)
    return flat_ids * capacity + slot_rank


def contract_rows(left, right):
    return lax.dot_general(
        left, right, (((0,), (0,)), ((), ())), preferred_element_type=jnp.float32
    )


def body(
    cotangent,
    mixer_out,
    route_ids,
    route_weights,
    conv_out,
    recur_gate,
    input_gate,
    gate_pre,
    states_before,
    decay_rate,
    out_proj,
    recur_map,
    input_map,
    expert_gate,
    expert_up,
    expert_down,
):
    row_count = cotangent.shape[0]
    experts = lax.axis_size("sp")
    capacity = 4 * row_count // experts
    slot_pos = route_slots(route_ids, experts, capacity).reshape(row_count, 2)
    slot_range = jnp.arange(experts * capacity, dtype=jnp.int32)[:, None]
    hit_first = slot_range == slot_pos[None, :, 0]
    hit_second = slot_range == slot_pos[None, :, 1]
    dispatch = (hit_first | hit_second).astype(jnp.bfloat16)
    slot_weight = jnp.sum(
        jnp.where(hit_first, route_weights[None, :, 0], 0.0)
        + jnp.where(hit_second, route_weights[None, :, 1], 0.0),
        axis=1,
    )
    send_rows = jnp.dot(dispatch, mixer_out, preferred_element_type=jnp.float32).astype(
        jnp.bfloat16
    )
    send_cot = (
        jnp.dot(dispatch, cotangent, preferred_element_type=jnp.float32) * slot_weight[:, None]
    ).astype(jnp.bfloat16)
    tps = lax.axis_size("tp")
    features = tps * cotangent.shape[1]
    slots = experts * capacity
    blocks = (experts, capacity, features)
    got_rows, got_cot = call(
        functools.partial(dispatch_kernel, experts, tps),
        [jax.ShapeDtypeStruct(blocks, jnp.bfloat16)] * 2,
        [
            DMA((2,)),
            DMA((2, experts)),
            DMA((2, experts)),
            DMA((2, experts, tps)),
            DMA((2, experts, tps)),
        ],
        0,
        send_rows.reshape(experts, capacity, -1),
        send_cot.reshape(experts, capacity, -1),
    )
    got_rows, got_cot = (got_rows.reshape(slots, features), got_cot.reshape(slots, features))
    w_gate = expert_gate[0]
    w_up = expert_up[0]
    w_down = expert_down[0]
    pre_gate = jnp.dot(got_rows, w_gate, preferred_element_type=jnp.float32)
    pre_up = jnp.dot(got_rows, w_up, preferred_element_type=jnp.float32)
    gate_act, slope = silu_parts(pre_gate)
    active = (gate_act * pre_up).astype(jnp.bfloat16)
    d_active = lax.dot_general(
        got_cot, w_down, (((1,), (1,)), ((), ())), preferred_element_type=jnp.float32
    )
    grad_down = contract_rows(active, got_cot).astype(jnp.bfloat16)
    d_gate = (d_active * pre_up * slope).astype(jnp.bfloat16)
    d_up = (d_active * gate_act).astype(jnp.bfloat16)
    grad_gate = contract_rows(got_rows, d_gate).astype(jnp.bfloat16)
    grad_up = contract_rows(got_rows, d_up).astype(jnp.bfloat16)
    partial_grad = lax.dot_general(
        d_gate, w_gate, (((1,), (1,)), ((), ())), preferred_element_type=jnp.float32
    ) + lax.dot_general(d_up, w_up, (((1,), (1,)), ((), ())), preferred_element_type=jnp.float32)
    channels = conv_out.shape[1]
    rate = decay_rate[None, :]
    recur_f = recur_gate.astype(jnp.float32)
    input_f = input_gate.astype(jnp.float32)
    conv_f = conv_out.astype(jnp.float32)
    before_f = states_before.astype(jnp.float32)
    log_decay = -8.0 * recur_f * rate
    decay_now = jnp.exp(log_decay)
    position = lax.axis_index("sp") * row_count + jnp.arange(row_count, dtype=jnp.int32)
    at_start = (position == 0)[:, None]
    norm_factor = jnp.where(at_start, 1.0, jnp.sqrt(-jnp.expm1(2.0 * log_decay)))
    norm_slope = jnp.where(at_start, 0.0, -jnp.exp(2.0 * log_decay) / norm_factor)
    drive = input_f * conv_f
    state = decay_now * before_f + norm_factor * drive
    gate, gelu_back = jax.vjp(jax.nn.gelu, gate_pre.astype(jnp.float32))
    mixed = (state * gate).astype(jnp.bfloat16)
    block = (experts, capacity, cotangent.shape[1])
    pair_sems, own_sems = (DMA((2,)), DMA((experts,)))
    tp_sems = DMA((tps,))
    out_grad, mixed_all = call(
        functools.partial(combine_kernel, experts, tps),
        [
            jax.ShapeDtypeStruct((row_count, features), jnp.bfloat16),
            jax.ShapeDtypeStruct((experts, row_count, channels), jnp.bfloat16),
        ],
        [
            pltpu.VMEM((2, *block), jnp.bfloat16),
            pltpu.VMEM(block, jnp.bfloat16),
            pltpu.VMEM(block, jnp.bfloat16),
            pltpu.VMEM(block, jnp.bfloat16),
            pltpu.VMEM(block, jnp.bfloat16),
            DMA,
            pair_sems,
            pair_sems,
            *([own_sems] * 6),
            tp_sems,
            tp_sems,
        ],
        1,
        partial_grad.astype(jnp.bfloat16).reshape(blocks),
        mixed,
        cotangent,
        dispatch.reshape(experts, capacity, row_count),
    )
    d_mixed = jnp.dot(out_grad, out_proj, preferred_element_type=jnp.float32)
    state_grad, pieces = call(
        functools.partial(scan_kernel, experts),
        [
            jax.ShapeDtypeStruct((row_count, channels), jnp.float32),
            jax.ShapeDtypeStruct((features // experts, experts * row_count), jnp.bfloat16),
        ],
        [
            pltpu.VMEM((row_count, channels), jnp.float32),
            pltpu.VMEM((2, channels), jnp.float32),
            pltpu.VMEM((experts, 2, channels), jnp.float32),
            DMA,
            *([own_sems] * 4),
        ],
        2,
        out_grad.T,
        d_mixed * gate,
        decay_now,
    )
    grad_out_proj = jnp.dot(
        pieces,
        mixed_all.reshape(experts * row_count, channels),
        preferred_element_type=jnp.float32,
    )
    grad_gate_pre = gelu_back(d_mixed * state)[0].astype(jnp.bfloat16)
    d_log = state_grad * (decay_now * before_f + norm_slope * drive)
    d_recur_pre = (d_log * (-8.0 * rate) * recur_f * (1.0 - recur_f)).astype(jnp.bfloat16)
    d_input_pre = (state_grad * norm_factor * conv_f * input_f * (1.0 - input_f)).astype(
        jnp.bfloat16
    )
    groups = recur_map.shape[0]
    width = recur_map.shape[1]
    through_recur = jnp.einsum(
        "tbj,bij->tbi",
        d_recur_pre.reshape(row_count, groups, width),
        recur_map,
        preferred_element_type=jnp.float32,
    )
    through_input = jnp.einsum(
        "tbj,bij->tbi",
        d_input_pre.reshape(row_count, groups, width),
        input_map,
        preferred_element_type=jnp.float32,
    )
    grad_conv = (
        state_grad * norm_factor * input_f
        + (through_recur + through_input).reshape(row_count, channels)
    ).astype(jnp.bfloat16)
    return (
        grad_gate[None],
        grad_up[None],
        grad_down[None],
        grad_out_proj,
        grad_conv,
        grad_gate_pre,
    )


def solution(mesh):
    placed = (
        P("sp", "tp"),
        P("sp", "tp"),
        P("sp", None),
        P("sp", None),
        P("sp", "tp"),
        P("sp", "tp"),
        P("sp", "tp"),
        P("sp", "tp"),
        P("sp", "tp"),
        P("tp"),
        P(None, "tp"),
        P("tp", None, None),
        P("tp", None, None),
        P("sp", None, "tp"),
        P("sp", None, "tp"),
        P("sp", "tp", None),
    )
    return jax.shard_map(
        body,
        mesh=mesh,
        in_specs=placed,
        out_specs=(
            P("sp", None, "tp"),
            P("sp", None, "tp"),
            P("sp", "tp", None),
            P("sp", "tp"),
            P("sp", "tp"),
            P("sp", "tp"),
        ),
        check_vma=False,
    )
```

```python
import functools

import jax
import jax.numpy as jnp
from jax import lax
from jax.experimental import pallas as pl
from jax.experimental.pallas import tpu as pltpu
from jax.sharding import PartitionSpec as P

MESH = pl.DeviceIdType.MESH
VMEM = pl.BlockSpec(memory_space=pltpu.VMEM)
DMA = pltpu.SemaphoreType.DMA


def bits_of(count):
    found, bit = [], 1
    while bit < count:
        found.insert(0, bit)
        bit *= 2
    return found


def low_bit(mask):
    return mask & -mask


def flip(index, mask):
    bit = 1
    while bit <= mask:
        if mask & bit:
            index = index + bit - 2 * bit * lax.rem(lax.div(index, bit), 2)
        bit *= 2
    return index


def window(index, width):
    return pl.ds(pl.multiple_of(index * width, width), width)


def remote(source, target, send_sem, recv_sem, device):
    return pltpu.make_async_remote_copy(
        src_ref=source,
        dst_ref=target,
        send_sem=send_sem,
        recv_sem=recv_sem,
        device_id=device,
        device_id_type=MESH,
    )


def greet(peers):
    barrier = pltpu.get_barrier_semaphore()
    for peer in peers:
        pl.semaphore_signal(barrier, inc=1, device_id=peer, device_id_type=MESH)
    pl.semaphore_wait(barrier, len(peers))


def relays_of(count):
    masks = [mask for mask in range(1, count) if mask != low_bit(mask)]
    return sorted(masks, key=lambda mask: (bin(mask).count("1"), -mask))


def call(kernel, out_shape, scratch, ident, *operands):
    return pl.pallas_call(
        kernel,
        out_shape=out_shape,
        in_specs=[VMEM] * len(operands),
        out_specs=jax.tree.map(lambda _: VMEM, out_shape),
        scratch_shapes=scratch,
        compiler_params=pltpu.CompilerParams(
            collective_id=ident, has_side_effects=True, vmem_limit_bytes=48 * 1024 * 1024
        ),
    )(*operands)


def dispatch_kernel(n_sp, n_tp, rows, cots, got_rows, got_cots, own_sem, sa, ra, st, rt):
    s, t = lax.axis_index("sp"), lax.axis_index("tp")
    width = rows.shape[-1]
    kinds = ((rows, got_rows), (cots, got_cots))
    greet(
        [(flip(s, m), t) for m in range(1, n_sp)] + [(s, flip(t, b)) for b in bits_of(n_tp)]
    )

    def own(kind):
        source, target = kinds[kind]
        return pltpu.make_async_copy(
            source.at[s], target.at[s, :, window(t, width)], own_sem.at[kind]
        )

    def to_expert(kind, m):
        source, target = kinds[kind]
        q = flip(s, m)
        return remote(
            source.at[q], target.at[s, :, window(t, width)], sa.at[kind, m], ra.at[kind, m], (q, t)
        )

    def share(kind, m, k):
        bit = low_bit(k)
        block = kinds[kind][1].at[flip(s, m), :, window(flip(t, k - bit), width)]
        return remote(block, block, st.at[kind, m, k], rt.at[kind, m, k], (s, flip(t, bit)))

    seen = set()

    def forward(m):
        for kind in range(2):
            for k in relays_of(n_tp):
                before = k - low_bit(k)
                if (kind, m, before) not in seen:
                    share(kind, m, before).wait_recv()
                    seen.add((kind, m, before))
                share(kind, m, k).start()

    for kind in range(2):
        own(kind).start()
    for m in range(1, n_sp):
        for kind in range(2):
            to_expert(kind, m).start()
    for m in range(n_sp):
        for kind in range(2):
            if m == 0:
                own(kind).wait()
            else:
                to_expert(kind, m).wait_recv()
            for bit in bits_of(n_tp):
                share(kind, m, bit).start()
        if m > 0:
            forward(m - 1)
    forward(n_sp - 1)
    for kind in range(2):
        for m in range(n_sp):
            if m > 0:
                to_expert(kind, m).wait_send()
            for k in range(1, n_tp):
                share(kind, m, k).wait_send()
                if (kind, m, k) not in seen:
                    share(kind, m, k).wait_recv()


def combine_kernel(
    n_sp, n_tp, part, mixed, base, pick, out, mixed_all, half, xsend, xrecv, back, ret,
    own_sem, sh, rh, sx, rx, sb, rb, sg, rg, st, rt,
):
    s, t = lax.axis_index("sp"), lax.axis_index("tp")
    width = ret.shape[-1]
    pair, across = flip(t, 1), flip(t, 2)
    greet(
        [(flip(s, m), t) for m in range(1, n_sp)] + [(s, flip(t, b)) for b in bits_of(n_tp)]
    )

    def to_pair(slot):
        chunk = flip(pair, 2) if slot == 0 else pair
        return remote(
            part.at[:, :, window(chunk, width)], half.at[slot], sh.at[slot], rh.at[slot], (s, pair)
        )

    def cross(m):
        q = flip(s, m)
        return remote(xsend.at[q], xrecv.at[q], sx.at[m], rx.at[m], (s, across))

    def give(m):
        q = flip(s, m)
        return remote(back.at[q], ret.at[s], sb.at[m], rb.at[m], (q, t))

    def gather(k):
        bit = low_bit(k)
        block = flip(s, k - bit)
        source = mixed if k == bit else mixed_all.at[block]
        return remote(source, mixed_all.at[block], sg.at[k], rg.at[k], (flip(s, bit), t))

    seen = set()

    def forward(masks):
        for k in masks:
            before = k - low_bit(k)
            if before not in seen:
                gather(before).wait_recv()
                seen.add(before)
            gather(k).start()

    to_pair(0).start()
    to_pair(1).start()
    own = pltpu.make_async_copy(mixed, mixed_all.at[s], own_sem)
    own.start()
    for bit in bits_of(n_sp):
        gather(bit).start()
    order = list(range(n_sp - 1, -1, -1))
    to_pair(0).wait_recv()
    for m in order:
        q = flip(s, m)
        xsend[q] = (
            part[q, :, window(across, width)].astype(jnp.float32) + half[0, q].astype(jnp.float32)
        ).astype(jnp.bfloat16)
        cross(m).start()
    to_pair(1).wait_recv()
    relays = relays_of(n_sp)
    early = [k for k in relays if bin(k).count("1") == 2]
    forward(early)
    for place, m in enumerate(order):
        q = flip(s, m)
        cross(m).wait_recv()
        total = (
            part[q, :, window(t, width)].astype(jnp.float32)
            + half[1, q].astype(jnp.float32)
            + xrecv[q].astype(jnp.float32)
        ).astype(jnp.bfloat16)
        if m == 0:
            ret[s] = total
        else:
            back[q] = total
            give(m).start()
        if place == n_sp // 2:
            forward([k for k in relays if k not in early])
    total = base[...].astype(jnp.float32)
    for m in range(n_sp):
        q = flip(s, m)
        if m > 0:
            give(m).wait_recv()
        total = total + contract_rows(pick[q], ret[q])
    out[:, window(t, width)] = total.astype(jnp.bfloat16)

    def share(k):
        bit = low_bit(k)
        block = out.at[:, window(flip(t, k - bit), width)]
        return remote(block, block, st.at[k], rt.at[k], (s, flip(t, bit)))

    for bit in bits_of(n_tp):
        share(bit).start()
    shared = set()
    for k in relays_of(n_tp):
        before = k - low_bit(k)
        if before not in shared:
            share(before).wait_recv()
            shared.add(before)
        share(k).start()
    for k in range(1, n_tp):
        share(k).wait_send()
        if k not in shared:
            share(k).wait_recv()
    own.wait()
    for slot in range(2):
        to_pair(slot).wait_send()
    for m in range(n_sp):
        cross(m).wait_send()
        if m > 0:
            give(m).wait_send()
            gather(m).wait_send()
            if m not in seen:
                gather(m).wait_recv()


def scan_kernel(
    n_sp, flipped, drive, decay, state_grad, pieces, weight, carry, carries,
    own_sem, sa, ra, sc, rc,
):
    s, t = lax.axis_index("sp"), lax.axis_index("tp")
    rows = drive.shape[0]
    share = flipped.shape[0] // n_sp
    greet([(flip(s, m), t) for m in range(1, n_sp)])

    def piece(m):
        q = flip(s, m)
        return remote(
            flipped.at[window(q, share)], pieces.at[:, window(s, rows)], sa.at[m], ra.at[m], (q, t)
        )

    def send_carry(m):
        return remote(carry, carries.at[s], sc.at[m], rc.at[m], (flip(s, m), t))

    own = pltpu.make_async_copy(
        flipped.at[window(s, share)], pieces.at[:, window(s, rows)], own_sem
    )
    own.start()

    def lap(step, held):
        grad, product = held
        row = rows - 1 - step
        grad = drive[pl.ds(row, 1), :] + grad
        product_here = product
        state_grad[pl.ds(row, 1), :] = grad
        weight[pl.ds(row, 1), :] = product_here
        now = decay[pl.ds(row, 1), :]
        return (now * grad, now * product_here)

    zero = jnp.zeros((1, drive.shape[1]), jnp.float32)
    start, span = lax.fori_loop(0, rows, lap, (zero, zero + 1.0), unroll=8)
    carry[0:1, :] = span
    carry[1:2, :] = start
    for m in range(1, n_sp):
        send_carry(m).start()
    for m in range(1, n_sp):
        piece(m).start()
    for m in range(1, n_sp):
        send_carry(m).wait_recv()
    incoming = zero
    for later in range(n_sp - 1, 0, -1):
        longer = carries[later, 1:2, :] + carries[later, 0:1, :] * incoming
        incoming = jnp.where(later > s, longer, incoming)
    state_grad[...] = state_grad[...] + weight[...] * incoming
    own.wait()
    for m in range(1, n_sp):
        send_carry(m).wait_send()
        piece(m).wait_send()
        piece(m).wait_recv()


def silu_parts(values):
    sig = jax.nn.sigmoid(values)
    return (values * sig, sig * (1.0 + values * (1.0 - sig)))


def route_slots(route_block, experts, capacity):
    flat_ids = route_block.reshape(-1)
    onehot = (flat_ids[:, None] == jnp.arange(experts, dtype=jnp.int32)[None, :]).astype(jnp.int32)
    before = jnp.cumsum(onehot, axis=0) - onehot
    slot_rank = jnp.sum(before * onehot, axis=1)
    return flat_ids * capacity + slot_rank


def contract_rows(left, right):
    return lax.dot_general(
        left, right, (((0,), (0,)), ((), ())), preferred_element_type=jnp.float32
    )


def body(
    cotangent,
    mixer_out,
    route_ids,
    route_weights,
    conv_out,
    recur_gate,
    input_gate,
    gate_pre,
    states_before,
    decay_rate,
    out_proj,
    recur_map,
    input_map,
    expert_gate,
    expert_up,
    expert_down,
):
    row_count = cotangent.shape[0]
    experts = lax.axis_size("sp")
    capacity = 4 * row_count // experts
    slot_pos = route_slots(route_ids, experts, capacity).reshape(row_count, 2)
    slot_range = jnp.arange(experts * capacity, dtype=jnp.int32)[:, None]
    hit_first = slot_range == slot_pos[None, :, 0]
    hit_second = slot_range == slot_pos[None, :, 1]
    dispatch = (hit_first | hit_second).astype(jnp.bfloat16)
    slot_weight = jnp.sum(
        jnp.where(hit_first, route_weights[None, :, 0], 0.0)
        + jnp.where(hit_second, route_weights[None, :, 1], 0.0),
        axis=1,
    )
    send_rows = jnp.dot(dispatch, mixer_out, preferred_element_type=jnp.float32).astype(
        jnp.bfloat16
    )
    send_cot = (
        jnp.dot(dispatch, cotangent, preferred_element_type=jnp.float32) * slot_weight[:, None]
    ).astype(jnp.bfloat16)
    tps = lax.axis_size("tp")
    features = tps * cotangent.shape[1]
    slots = experts * capacity
    blocks = (experts, capacity, features)
    got_rows, got_cot = call(
        functools.partial(dispatch_kernel, experts, tps),
        [jax.ShapeDtypeStruct(blocks, jnp.bfloat16)] * 2,
        [
            DMA((2,)),
            DMA((2, experts)),
            DMA((2, experts)),
            DMA((2, experts, tps)),
            DMA((2, experts, tps)),
        ],
        0,
        send_rows.reshape(experts, capacity, -1),
        send_cot.reshape(experts, capacity, -1),
    )
    got_rows, got_cot = (got_rows.reshape(slots, features), got_cot.reshape(slots, features))
    w_gate = expert_gate[0]
    w_up = expert_up[0]
    w_down = expert_down[0]
    pre_gate = jnp.dot(got_rows, w_gate, preferred_element_type=jnp.float32)
    pre_up = jnp.dot(got_rows, w_up, preferred_element_type=jnp.float32)
    gate_act, slope = silu_parts(pre_gate)
    active = (gate_act * pre_up).astype(jnp.bfloat16)
    d_active = lax.dot_general(
        got_cot, w_down, (((1,), (1,)), ((), ())), preferred_element_type=jnp.float32
    )
    grad_down = contract_rows(active, got_cot).astype(jnp.bfloat16)
    d_gate = (d_active * pre_up * slope).astype(jnp.bfloat16)
    d_up = (d_active * gate_act).astype(jnp.bfloat16)
    grad_gate = contract_rows(got_rows, d_gate).astype(jnp.bfloat16)
    grad_up = contract_rows(got_rows, d_up).astype(jnp.bfloat16)
    partial_grad = lax.dot_general(
        d_gate, w_gate, (((1,), (1,)), ((), ())), preferred_element_type=jnp.float32
    ) + lax.dot_general(d_up, w_up, (((1,), (1,)), ((), ())), preferred_element_type=jnp.float32)
    channels = conv_out.shape[1]
    rate = decay_rate[None, :]
    recur_f = recur_gate.astype(jnp.float32)
    input_f = input_gate.astype(jnp.float32)
    conv_f = conv_out.astype(jnp.float32)
    before_f = states_before.astype(jnp.float32)
    log_decay = -8.0 * recur_f * rate
    decay_now = jnp.exp(log_decay)
    position = lax.axis_index("sp") * row_count + jnp.arange(row_count, dtype=jnp.int32)
    at_start = (position == 0)[:, None]
    norm_factor = jnp.where(at_start, 1.0, jnp.sqrt(-jnp.expm1(2.0 * log_decay)))
    norm_slope = jnp.where(at_start, 0.0, -jnp.exp(2.0 * log_decay) / norm_factor)
    drive = input_f * conv_f
    state = decay_now * before_f + norm_factor * drive
    gate, gelu_back = jax.vjp(jax.nn.gelu, gate_pre.astype(jnp.float32))
    mixed = (state * gate).astype(jnp.bfloat16)
    block = (experts, capacity, cotangent.shape[1])
    pair_sems, own_sems = (DMA((2,)), DMA((experts,)))
    tp_sems = DMA((tps,))
    out_grad, mixed_all = call(
        functools.partial(combine_kernel, experts, tps),
        [
            jax.ShapeDtypeStruct((row_count, features), jnp.bfloat16),
            jax.ShapeDtypeStruct((experts, row_count, channels), jnp.bfloat16),
        ],
        [
            pltpu.VMEM((2, *block), jnp.bfloat16),
            pltpu.VMEM(block, jnp.bfloat16),
            pltpu.VMEM(block, jnp.bfloat16),
            pltpu.VMEM(block, jnp.bfloat16),
            pltpu.VMEM(block, jnp.bfloat16),
            DMA,
            pair_sems,
            pair_sems,
            *([own_sems] * 6),
            tp_sems,
            tp_sems,
        ],
        1,
        partial_grad.astype(jnp.bfloat16).reshape(blocks),
        mixed,
        cotangent,
        dispatch.reshape(experts, capacity, row_count),
    )
    d_mixed = jnp.dot(out_grad, out_proj, preferred_element_type=jnp.float32)
    state_grad, pieces = call(
        functools.partial(scan_kernel, experts),
        [
            jax.ShapeDtypeStruct((row_count, channels), jnp.float32),
            jax.ShapeDtypeStruct((features // experts, experts * row_count), jnp.bfloat16),
        ],
        [
            pltpu.VMEM((row_count, channels), jnp.float32),
            pltpu.VMEM((2, channels), jnp.float32),
            pltpu.VMEM((experts, 2, channels), jnp.float32),
            DMA,
            *([own_sems] * 4),
        ],
        2,
        out_grad.T,
        d_mixed * gate,
        decay_now,
    )
    grad_out_proj = jnp.dot(
        pieces,
        mixed_all.reshape(experts * row_count, channels),
        preferred_element_type=jnp.float32,
    )
    grad_gate_pre = gelu_back(d_mixed * state)[0].astype(jnp.bfloat16)
    d_log = state_grad * (decay_now * before_f + norm_slope * drive)
    d_recur_pre = (d_log * (-8.0 * rate) * recur_f * (1.0 - recur_f)).astype(jnp.bfloat16)
    d_input_pre = (state_grad * norm_factor * conv_f * input_f * (1.0 - input_f)).astype(
        jnp.bfloat16
    )
    groups = recur_map.shape[0]
    width = recur_map.shape[1]
    through_recur = jnp.einsum(
        "tbj,bij->tbi",
        d_recur_pre.reshape(row_count, groups, width),
        recur_map,
        preferred_element_type=jnp.float32,
    )
    through_input = jnp.einsum(
        "tbj,bij->tbi",
        d_input_pre.reshape(row_count, groups, width),
        input_map,
        preferred_element_type=jnp.float32,
    )
    grad_conv = (
        state_grad * norm_factor * input_f
        + (through_recur + through_input).reshape(row_count, channels)
    ).astype(jnp.bfloat16)
    return (
        grad_gate[None],
        grad_up[None],
        grad_down[None],
        grad_out_proj,
        grad_conv,
        grad_gate_pre,
    )


def solution(mesh):
    placed = (
        P("sp", "tp"),
        P("sp", "tp"),
        P("sp", None),
        P("sp", None),
        P("sp", "tp"),
        P("sp", "tp"),
        P("sp", "tp"),
        P("sp", "tp"),
        P("sp", "tp"),
        P("tp"),
        P(None, "tp"),
        P("tp", None, None),
        P("tp", None, None),
        P("sp", None, "tp"),
        P("sp", None, "tp"),
        P("sp", "tp", None),
    )
    return jax.shard_map(
        body,
        mesh=mesh,
        in_specs=placed,
        out_specs=(
            P("sp", None, "tp"),
            P("sp", None, "tp"),
            P("sp", "tp", None),
            P("sp", "tp"),
            P("sp", "tp"),
            P("sp", "tp"),
        ),
        check_vma=False,
    )
```
